128 devices in a mesh: sp: 64 (over z, y, x), tp: 2 (over core).
Axes of the slice: x: 4, y: 4, z: 4, core: 2. Of those that a mesh axis runs over, the one named last changes fastest.
Arguments:
- mixer_value_rows: bfloat16 [16384, 2048], P('sp', 'tp'), may hold values from -6 to 6
- input_map_rows: bfloat16 [16384, 256], P('sp', 'tp'), may hold values from -6 to 6
- output_map_rows: bfloat16 [16384, 256], P('sp', 'tp'), may hold values from -6 to 6
- gate_preactivation: bfloat16 [16384, 2048], P('sp', 'tp'), may hold values from -25 to 25
- step_preactivation: float32 [16384, 32], P('sp', 'tp'), may hold values from -4 to 4
- position_extra_decay: float32 [16384, 32], P('sp', 'tp'), may hold values from -0.69 to 0
- head_decay_rate: float32 [32], P('tp'), may hold values from 7.8125e-05 to 0.08
- head_direct_term: float32 [32], P('tp'), may hold values from -2.5 to 2.5
- value_taps: bfloat16 [4, 2048], P(None, 'tp'), may hold values from -3 to 3
- input_map_taps: bfloat16 [4, 256], P(None, 'tp'), may hold values from -3 to 3
- output_map_taps: bfloat16 [4, 256], P(None, 'tp'), may hold values from -3 to 3
- document_index: int32 [16384], P('sp'), may hold values from 0 to 15, never falling along the last dimension, each value on 1 to 1536 neighbouring positions
- gated_norm_gain: float32 [2048], replicated, may hold values from 0.1 to 1.9
- residual: bfloat16 [16384, 2048], P(('sp', 'tp')), may hold values from -6 to 6
- mixer_output_weight: bfloat16 [2048, 2048], replicated, may hold values from -0.125 to 0.125
- expert_norm_gain: float32 [2048], replicated, may hold values from 0.1 to 1.9
- expert_group_weight: float32 [16384, 4], P(('sp', 'tp')), may hold values from 0.5 to 2
- chosen_expert_weight: float32 [16384, 2], P(('sp', 'tp')), may hold values from 0.5 to 2
- chosen_expert_index: int32 [16384, 2], P(('sp', 'tp')), may hold values from 0 to 127, all different within a row; in each aligned block of 128 rows (0 to 127, 128 to 255, ...) at most 4 rows name the same one
- expert_gate_weight: bfloat16 [128, 2048, 512], P(('sp', 'tp')), may hold values from -0.125 to 0.125
- expert_up_weight: bfloat16 [128, 2048, 512], P(('sp', 'tp')), may hold values from -0.125 to 0.125
- expert_down_weight: bfloat16 [128, 512, 2048], P(('sp', 'tp')), may hold values from -0.25 to 0.25
Outputs:
- output: bfloat16 [16384, 2048], P(('sp', 'tp'))
The draws below stay inside these ranges and needn't reach their ends.
Inputs may be any that keep to these rules, and one draw needn't show every extreme that they name: `document_index`: document numbers never fall along the sequence; a document holds 1 to 1536 positions. `chosen_expert_index`: the 2 entries of a row differ. Among the rows of one device (aligned blocks of 128 rows) no expert is named by more than 4 rows, a bound that some expert reaches in some blocks.
All inputs are finite; a program needn't handle non-finite values.
Results may differ from the reference program's by a relative error of at most 0.019.
Values may be sent and summed in bfloat16 or wider, within the bound.
No kernel may reach another device: no remote copies, remote signals or barrier semaphores. Data moves between devices by JAX's collectives and lax.ppermute only.
A program may use at most 128 MiB of HBM per device.

```python
import math
import jax
import jax.numpy as jnp
import numpy as np
from jax import lax

D = 2048
D_SSM = 2048
HEADS = 32
HEAD_DIM = 64
SSM_GROUPS = 2
D_STATE = 128
CONV_K = 4
BLOCK = 128
D_EXPERT = 512
EXPERT_GROUPS = 4
TOP = 2
TOK_DEV = 256
TOKENS = 16384
ROWS_DEV = 128
EXPERTS = 128
CAP = 4
N_SP = 64
N_TP = 2


def draw_gate_preactivation(key, part):
    position = jnp.arange(D_SSM, dtype=jnp.float32) / D_SSM
    scales = jnp.exp(1.6 * position)[None, :]
    values = jnp.clip(jax.random.normal(key, (TOKENS, D_SSM), jnp.float32), -4.9, 4.9)
    return (values * scales).astype(jnp.bfloat16)


def draw_step_preactivation(key, part):
    first, second = jax.random.split(key)
    blocks = TOKENS // TOK_DEV
    offsets = jax.random.uniform(second, (blocks, 1, 1), jnp.float32, -1.0, 1.0)
    noise = 0.7 * jnp.clip(jax.random.normal(first, (blocks, TOK_DEV, HEADS), jnp.float32), -4.0, 4.0)
    return (noise + offsets).reshape(TOKENS, HEADS)


def draw_head_decay_rate(key, part):
    first, second, third = jax.random.split(key, 3)
    share = 0.5
    slow_mask = jax.random.uniform(first, (HEADS,), jnp.float32) < share
    slow_rate = jnp.exp(jax.random.uniform(second, (HEADS,), jnp.float32, jnp.log(0.021 / TOK_DEV), jnp.log(0.2 / TOK_DEV)))
    fast_rate = jnp.exp(jax.random.uniform(third, (HEADS,), jnp.float32, jnp.log(0.021), jnp.log(0.079)))
    return jnp.where(slow_mask, slow_rate, fast_rate)


def draw_position_extra_decay(key, part):
    first, second = jax.random.split(key)
    hits = (jax.random.uniform(first, (TOKENS, 1), jnp.float32) < 24.0 / TOKENS).astype(jnp.float32)
    depth = jax.random.uniform(second, (TOKENS, HEADS), jnp.float32, 0.35, 0.69)
    return -depth * hits


def block_levels(own_key, extent, cuts, smallest, top_value):
    gain, own = 1.0, jax.random.fold_in(own_key, 6)
    for axis_at, blocks in cuts:
        heights = jnp.exp(jax.random.uniform(jax.random.fold_in(own, axis_at), (blocks,), jnp.float32, smallest / len(cuts), top_value / len(cuts)))
        gain = gain * jnp.repeat(heights, extent[axis_at] // blocks).reshape([-1 if axis == axis_at else 1 for axis in range(len(extent))])
    return gain


def split_up(number_of, total, reach, lean):
    loads = [(1 << 20) // math.isqrt(grade ** lean) + 1 for grade in range(2, number_of + 1)]
    rest, counts = total - reach - (number_of - 1), [1] * (number_of - 1)
    while rest > 0:
        movable = [i for i in range(number_of - 1) if counts[i] < reach]
        mass, left = sum([loads[i] for i in movable]), rest
        for i in movable:
            more = min(reach - counts[i], max(1, left * loads[i] // mass), rest)
            counts[i] = counts[i] + more
            rest = rest - more
    return np.array([reach] + counts)


def ragged(rng, amount, total, reach, lean):
    if amount == 2:
        one = jax.random.randint(rng, (), max(1, total - reach), min(reach, total - 1) + 1)
        return jnp.stack([one, total - one])
    tallies = jnp.asarray(split_up(amount, total, reach, lean), jnp.int32)
    couples = (amount - 1) // 2
    source_of, sink = tallies[1:1 + 2 * couples:2], tallies[2:2 + 2 * couples:2]
    margin = jnp.minimum(source_of - 1, reach - sink)
    moved = jax.random.randint(jax.random.fold_in(rng, 1), (couples,), 0, 1 << 20) % (margin + 1)
    tallies = tallies.at[1:1 + 2 * couples:2].set(source_of - moved).at[2:2 + 2 * couples:2].set(sink + moved)
    return tallies[jax.random.permutation(jax.random.fold_in(rng, 2), amount)]


def assign_block(key, own, number, rows, count, top, most, skew):
    sequence = jax.random.permutation(key, count)
    crowded, common = portions_of(count, rows * top, most, skew, True), portions_of(count, rows * top, most, skew, False)
    places = jnp.arange(count)

    def named(lengths, offset_by):
        used = int((lengths > 0).sum())
        fixed = max(1, used // 4)
        passed = fixed + (places - fixed + offset_by * (used - fixed)) % max(1, count - fixed)
        return jnp.zeros((count,), jnp.int32).at[sequence[jnp.where(places < fixed, places, passed)]].set(jnp.asarray(lengths, jnp.int32))

    lengths = jnp.where(number % 4 == 0, named(crowded, number // 4), named(common, number - number // 4 - 1))
    mixed = jax.random.permutation(jax.random.fold_in(own, 3), count)
    giver, receiver = mixed[0:count // 2 * 2:2], mixed[1:count // 2 * 2:2]
    slack = jnp.minimum(lengths[giver] - 1, most - lengths[receiver]) // 2
    slack = jnp.where((giver == sequence[0]) | (receiver == sequence[0]) | (lengths[receiver] == 0), 0, jnp.maximum(slack, 0))
    passed = jax.random.randint(jax.random.fold_in(own, 4), (count // 2,), 0, 1 << 20) % (slack + 1)
    lengths = lengths.at[giver].add(-passed).at[receiver].add(passed)
    members = jnp.searchsorted(jnp.cumsum(lengths), jnp.arange(rows * top), side="right").astype(jnp.int32)
    listing = members.reshape(top, rows).T
    listing = listing[jax.random.permutation(jax.random.fold_in(own, 1), rows)]
    offset_by = jax.random.randint(jax.random.fold_in(own, 2), (rows, 1), 0, top)
    return jnp.take_along_axis(listing, (jnp.arange(top)[None, :] + offset_by) % top, axis=1)


def portions_of(amount, total, limit, lean, full):
    portions = [(1 << 20) // math.isqrt(rank ** lean) + 1 for rank in range(1, amount + 1)]
    largest = limit if full else min(limit, max(-(-total // amount), total * portions[0] // sum(portions)))
    least = 1 if total - largest >= amount - 1 else 0
    holding, rest = [largest] + [least] * (amount - 1), total - largest - least * (amount - 1)
    while rest > 0:
        candidates = [i for i in range(1, amount) if holding[i] < largest] or [i for i in range(1, amount) if holding[i] < limit]
        pool, remaining = sum([portions[i] for i in candidates]), rest
        for i in candidates:
            more = min(limit - holding[i], max(1, remaining * portions[i] // pool), rest)
            holding[i] = holding[i] + more
            rest = rest - more
    return np.array(holding)


def centred(stream_key, dims, width, limit, cuts=(), kind=jnp.bfloat16):
    drawn = width * jax.random.normal(stream_key, dims, jnp.float32)
    if cuts:
        drawn = drawn * block_levels(stream_key, dims, cuts, -0.22, 0.18)
    return jnp.clip(drawn, -limit, limit).astype(kind)


def setup_inputs(seed: int = 0) -> dict:
    key_of = jax.random.split(jax.random.key(seed), 23)
    mixer_value_rows = centred(key_of[0], (TOKENS, D_SSM), 1.0, 6.0, ((0, 64), (1, 2)))
    input_map_rows = centred(key_of[1], (TOKENS, SSM_GROUPS * D_STATE), 1.0, 6.0, ((0, 64), (1, 2)))
    output_map_rows = centred(key_of[2], (TOKENS, SSM_GROUPS * D_STATE), 1.0, 6.0, ((0, 64), (1, 2)))
    gate_preactivation = draw_gate_preactivation(jax.random.fold_in(key_of[22], 71), 0)
    step_preactivation = draw_step_preactivation(jax.random.fold_in(key_of[22], 71), 0)
    position_extra_decay = draw_position_extra_decay(jax.random.fold_in(key_of[22], 71), 0)
    head_decay_rate = draw_head_decay_rate(jax.random.fold_in(key_of[22], 71), 0)
    head_direct_term = jnp.clip(jax.random.uniform(key_of[7], (HEADS,), jnp.float32, -2.5, 2.5) * block_levels(key_of[7], (HEADS,), ((0, 2),), -0.4, 0.0), -2.5, 2.5)
    value_taps = centred(key_of[8], (CONV_K, D_SSM), CONV_K ** -0.5, 3.0, ((1, 2),))
    input_map_taps = centred(key_of[9], (CONV_K, SSM_GROUPS * D_STATE), CONV_K ** -0.5, 3.0, ((1, 2),))
    output_map_taps = centred(key_of[10], (CONV_K, SSM_GROUPS * D_STATE), CONV_K ** -0.5, 3.0, ((1, 2),))
    document_index = jnp.searchsorted(jnp.cumsum(ragged(key_of[11], N_SP // 4, TOKENS, 6 * TOK_DEV, 1)), jnp.arange(TOKENS), side="right").astype(jnp.int32)
    gated_norm_gain = jnp.clip(1.0 + 0.18 * jax.random.normal(key_of[12], (D_SSM,), jnp.float32), 0.1, 1.9)
    residual = centred(key_of[13], (TOKENS, D), 1.0, 6.0, ((0, 128),))
    mixer_output_weight = centred(key_of[14], (D_SSM, D), D_SSM ** -0.5, 0.125)
    expert_norm_gain = jnp.clip(1.0 + 0.18 * jax.random.normal(key_of[15], (D,), jnp.float32), 0.1, 1.9)
    expert_group_weight = jnp.clip(0.5 + 1.5 * jax.random.uniform(key_of[16], (TOKENS, EXPERT_GROUPS), jnp.float32) ** block_levels(key_of[16], (TOKENS, EXPERT_GROUPS), ((0, 128),), -0.2, 0.2), 0.5, 2.0)
    chosen_expert_weight = jnp.clip(0.5 + 1.5 * jax.random.uniform(key_of[17], (TOKENS, TOP), jnp.float32) ** block_levels(key_of[17], (TOKENS, TOP), ((0, 128),), -0.2, 0.2), 0.5, 2.0)
    chosen_expert_index_keys = jax.random.split(jax.random.fold_in(key_of[18], 1), TOKENS // ROWS_DEV)
    chosen_expert_index_turns = jax.random.permutation(jax.random.fold_in(key_of[18], 3), TOKENS // ROWS_DEV)
    chosen_expert_index = jax.vmap(lambda own, number: assign_block(jax.random.fold_in(key_of[18], 2), own, number, ROWS_DEV, EXPERTS, TOP, CAP, 1))(chosen_expert_index_keys, chosen_expert_index_turns).reshape((TOKENS, TOP))
    expert_gate_weight = centred(key_of[19], (EXPERTS, D, D_EXPERT), D ** -0.5, 0.125, ((0, 128),))
    expert_up_weight = centred(key_of[20], (EXPERTS, D, D_EXPERT), D ** -0.5, 0.125, ((0, 128),))
    expert_down_weight = centred(key_of[21], (EXPERTS, D_EXPERT, D), D_EXPERT ** -0.5, 0.25, ((0, 128),))
    return dict(mixer_value_rows=mixer_value_rows, input_map_rows=input_map_rows, output_map_rows=output_map_rows, gate_preactivation=gate_preactivation, step_preactivation=step_preactivation, position_extra_decay=position_extra_decay, head_decay_rate=head_decay_rate, head_direct_term=head_direct_term, value_taps=value_taps, input_map_taps=input_map_taps, output_map_taps=output_map_taps, document_index=document_index, gated_norm_gain=gated_norm_gain, residual=residual, mixer_output_weight=mixer_output_weight, expert_norm_gain=expert_norm_gain, expert_group_weight=expert_group_weight, chosen_expert_weight=chosen_expert_weight, chosen_expert_index=chosen_expert_index, expert_gate_weight=expert_gate_weight, expert_up_weight=expert_up_weight, expert_down_weight=expert_down_weight)


EPSILON = 1e-06

def conv_silu(source_rows, weights, documents):
    kernel = weights.shape[0]
    length = source_rows.shape[0]
    padded = jnp.concatenate([jnp.zeros((kernel - 1, source_rows.shape[1]), jnp.float32), source_rows.astype(jnp.float32)], axis=0)
    pad_docs = jnp.concatenate([jnp.full((kernel - 1,), -1, jnp.int32), documents])
    summed = jnp.zeros((length, source_rows.shape[1]), jnp.float32)
    for offset in range(kernel):
        same_doc = (pad_docs[offset:offset + length] == documents).astype(jnp.float32)
        summed = summed + weights[offset].astype(jnp.float32)[None, :] * padded[offset:offset + length] * same_doc[:, None]
    return jax.nn.silu(summed).astype(jnp.bfloat16)

def scaled_norm(values, gain_vector):
    widened = values.astype(jnp.float32)
    factor = lax.rsqrt(lax.optimization_barrier(jnp.mean(widened * widened, axis=-1, keepdims=True)) + EPSILON)
    return (widened * factor * gain_vector.astype(jnp.float32)[None, :]).astype(jnp.bfloat16)

def block_step(carried_pair, pieces):
    carried, last_doc = carried_pair
    step_values, decay_block, b_block, c_block, doc_block = pieces
    length = step_values.shape[0]
    cumulative = jnp.cumsum(decay_block, axis=0)
    causal = jnp.arange(length)[:, None] >= jnp.arange(length)[None, :]
    allowed = causal & (doc_block[:, None] == doc_block[None, :])
    cum_heads = jnp.transpose(cumulative, (1, 2, 0))
    spread = cum_heads[:, :, :, None] - cum_heads[:, :, None, :]
    kernel_mat = jnp.exp(jnp.where(allowed[None, None], spread, -jnp.inf))
    scores = jnp.einsum('lgn,sgn->gls', c_block, b_block, preferred_element_type=jnp.float32)
    weighted = (scores[:, None] * kernel_mat).astype(jnp.bfloat16)
    inside = jnp.einsum('grls,sgrp->lgrp', weighted, step_values, preferred_element_type=jnp.float32)
    entering = (doc_block == last_doc).astype(jnp.float32)
    readout = jnp.einsum('lgn,grpn->lgrp', c_block, carried.astype(jnp.bfloat16), preferred_element_type=jnp.float32)
    inside = inside + readout * (jnp.exp(cumulative) * entering[:, None, None])[..., None]
    tail_mask = (doc_block == doc_block[-1]).astype(jnp.float32)
    end_decay = jnp.exp(cumulative[-1][None] - cumulative) * tail_mask[:, None, None]
    end_values = (end_decay[..., None] * step_values.astype(jnp.float32)).astype(jnp.bfloat16)
    fresh_state = jnp.einsum('lgn,lgrp->grpn', b_block, end_values, preferred_element_type=jnp.float32)
    keep_flag = (doc_block[-1] == last_doc).astype(jnp.float32)
    fresh_state = fresh_state + carried * (jnp.exp(cumulative[-1]) * keep_flag)[..., None, None]
    return ((fresh_state, doc_block[-1]), inside)

def state_mixer(value_conv, input_conv, output_conv, head_step_length, decay_logarithm, documents, head_direct_term):
    length = value_conv.shape[0]
    blocks = length // BLOCK
    per_group = HEADS // SSM_GROUPS
    value_heads = value_conv.astype(jnp.float32).reshape(length, SSM_GROUPS, per_group, HEAD_DIM)
    step_values = (value_heads * head_step_length.reshape(length, SSM_GROUPS, per_group)[..., None]).astype(jnp.bfloat16)
    decay_heads = decay_logarithm.reshape(blocks, BLOCK, SSM_GROUPS, per_group)
    input_groups = input_conv.reshape(blocks, BLOCK, SSM_GROUPS, D_STATE)
    output_groups = output_conv.reshape(blocks, BLOCK, SSM_GROUPS, D_STATE)
    doc_blocks = documents.reshape(blocks, BLOCK)
    initial = (jnp.zeros((SSM_GROUPS, per_group, HEAD_DIM, D_STATE), jnp.float32), jnp.array(-1, jnp.int32))
    ended, outputs = lax.scan(block_step, initial, (step_values.reshape(blocks, BLOCK, SSM_GROUPS, per_group, HEAD_DIM), decay_heads, input_groups, output_groups, doc_blocks))
    outputs = outputs.reshape(length, SSM_GROUPS, per_group, HEAD_DIM) + value_heads * head_direct_term.reshape(SSM_GROUPS, per_group)[None, :, :, None]
    return outputs.reshape(length, HEADS * HEAD_DIM)

def reference(mixer_value_rows, input_map_rows, output_map_rows, gate_preactivation, step_preactivation, position_extra_decay, head_decay_rate, head_direct_term, value_taps, input_map_taps, output_map_taps, document_index, gated_norm_gain, residual, mixer_output_weight, expert_norm_gain, expert_group_weight, chosen_expert_weight, chosen_expert_index, expert_gate_weight, expert_up_weight, expert_down_weight):
    documents = document_index.astype(jnp.int32)
    value_conv = conv_silu(mixer_value_rows, value_taps, documents)
    input_conv = conv_silu(input_map_rows, input_map_taps, documents)
    output_conv = conv_silu(output_map_rows, output_map_taps, documents)
    head_step_length = jax.nn.softplus(step_preactivation.astype(jnp.float32))
    decay_logarithm = position_extra_decay.astype(jnp.float32) - head_step_length * head_decay_rate.astype(jnp.float32)[None, :]
    mixer_out = state_mixer(value_conv, input_conv, output_conv, head_step_length, decay_logarithm, documents, head_direct_term.astype(jnp.float32))
    gated_rows = (mixer_out * jax.nn.silu(gate_preactivation.astype(jnp.float32))).astype(jnp.bfloat16)
    normed = scaled_norm(gated_rows, gated_norm_gain)
    mixed_rows = (residual.astype(jnp.float32) + jnp.dot(normed, mixer_output_weight, preferred_element_type=jnp.float32)).astype(jnp.bfloat16)
    ffn_in = scaled_norm(mixed_rows, expert_norm_gain)
    devices = N_SP * N_TP
    rows_dev = TOK_DEV // N_TP
    flat_ids = chosen_expert_index.astype(jnp.int32).reshape(devices, rows_dev * TOP)
    onehot = (flat_ids[:, :, None] == jnp.arange(EXPERTS, dtype=jnp.int32)[None, None, :]).astype(jnp.int32)
    ranking = lax.optimization_barrier(jnp.sum((jnp.cumsum(onehot, axis=1) - onehot) * onehot, axis=2))
    source = jnp.arange(devices, dtype=jnp.int32)[:, None]
    slot_index = (flat_ids * (devices * CAP) + source * CAP + ranking).reshape(-1)
    owners = jnp.arange(TOKENS * TOP, dtype=jnp.int32) // TOP
    slot_owner = jnp.zeros((EXPERTS * devices * CAP,), jnp.int32).at[slot_index].set(owners)
    slot_owner = slot_owner.reshape(EXPERTS, devices * CAP)

    def run_expert(pieces):
        indices, gate_matrix, up_matrix, down_matrix = pieces
        picked = ffn_in[indices]
        gate_part = jnp.dot(picked, gate_matrix, preferred_element_type=jnp.float32)
        upward = jnp.dot(picked, up_matrix, preferred_element_type=jnp.float32)
        hidden = (jax.nn.silu(gate_part) * upward).astype(jnp.bfloat16)
        return jnp.dot(hidden, down_matrix, preferred_element_type=jnp.float32).astype(jnp.bfloat16)
    results = lax.map(run_expert, (slot_owner, expert_gate_weight, expert_up_weight, expert_down_weight))
    gathered = results.reshape(-1, D)[slot_index].reshape(TOKENS, TOP, D)
    per_expert_group = EXPERTS // EXPERT_GROUPS
    owner_group = chosen_expert_index.astype(jnp.int32) // per_expert_group
    group_pick = (owner_group[:, :, None] == jnp.arange(EXPERT_GROUPS, dtype=jnp.int32)[None, None, :]).astype(jnp.float32)
    route_weight = lax.optimization_barrier(jnp.sum(group_pick * expert_group_weight[:, None, :], axis=2)) * chosen_expert_weight
    summed = mixed_rows.astype(jnp.float32) + lax.optimization_barrier(jnp.sum(route_weight[:, :, None] * gathered.astype(jnp.float32), axis=1))
    return summed.astype(jnp.bfloat16)
```

```python
import functools

import jax
import jax.numpy as jnp
from jax import lax
from jax.experimental import pallas as pl
from jax.experimental.pallas import tpu as pltpu
from jax.sharding import Mesh
from jax.sharding import PartitionSpec as P

SP = ("sp_0", "sp_1", "sp_2")
SP_TP = ("sp_0", "sp_1", "sp_2", "tp")
ROW = "sp_2"

EPS = 1e-06
LEN = 256
BLK = 128
CH = 1024
HEADS = 16
HD = 64
NS = 128
D = 2048
EXPERTS = 128
CAP = 4
QW = 512
HID = 512
SLOTS = EXPERTS * CAP
PAY = 136
NEG = -1e30
F32 = jnp.float32
BF16 = jnp.bfloat16
HIGH = lax.Precision.HIGHEST


def vmem(n):
    return [pl.BlockSpec(memory_space=pltpu.VMEM)] * n


def call(body, outs, n_in, scratch=(), limit=32, cost=None, in_specs=None, name=None):
    return pl.pallas_call(
        body,
        out_shape=outs,
        in_specs=in_specs or vmem(n_in),
        out_specs=jax.tree.map(lambda _: pl.BlockSpec(memory_space=pltpu.VMEM), outs),
        scratch_shapes=list(scratch),
        compiler_params=pltpu.CompilerParams(vmem_limit_bytes=limit * 1024 * 1024),
        cost_estimate=cost,
        name=name,
    )


def sds(shape, dtype):
    return jax.ShapeDtypeStruct(shape, dtype)


def iota(shape, dim):
    return lax.broadcasted_iota(jnp.int32, shape, dim)


def mm(a, b, precision=None):
    return jnp.dot(a, b, preferred_element_type=F32, precision=precision)


def softplus(v):
    return jnp.maximum(v, 0.0) + jnp.log(1.0 + jnp.exp(-jnp.abs(v)))


def silu(v):
    return v / (1.0 + jnp.exp(-v))


def head_expand():
    return (iota((HEADS, CH), 1) // HD == iota((HEADS, CH), 0)).astype(F32)


def split2(v):
    hi = v.astype(BF16)
    return hi, (v - hi.astype(F32)).astype(BF16)


def logs(step_ref, extra_ref, rate_ref):
    step = softplus(step_ref[...])
    return step, extra_ref[...] - step * rate_ref[...]


def cumulated(logd):
    tri = (iota((LEN, LEN), 0) >= iota((LEN, LEN), 1)).astype(F32)
    return mm(tri, logd, HIGH)


def conv(pad_ref, taps, masks, lo, width):
    acc = pad_ref[8 : 8 + LEN, lo : lo + width] * taps[3:4, lo : lo + width]
    for k in range(3):
        term = pad_ref[5 + k : 5 + k + LEN, lo : lo + width] * taps[k : k + 1, lo : lo + width]
        acc = acc + term * masks[k][:, :1]
    return silu(acc).astype(BF16)


def conv_kernel(
    values, bmap, cmap, edges, docs, step_pre, extra, rate, vtaps, btaps, ctaps,
    pay, xs_out, vc_out, bc_out, cc_out,
    vpad, mpad, dpad,
):
    vpad[0:8, :] = edges[:, 0:CH].astype(F32)
    vpad[8:, :] = values[...].astype(F32)
    mpad[0:8, :] = edges[:, CH : CH + 2 * NS].astype(F32)
    mpad[8:, 0:NS] = bmap[...].astype(F32)
    mpad[8:, NS:] = cmap[...].astype(F32)
    dpad[0:8, :] = edges[:, CH + 2 * NS :].astype(F32)
    dpad[8:, :] = docs[...]
    own = dpad[8:, :]
    masks = [(dpad[5 + k : 5 + k + LEN, :] == own).astype(F32) for k in range(3)]
    step, logd = logs(step_pre, extra, rate)
    cum = cumulated(logd)
    total = cum[LEN - 1 : LEN, :]
    last = dpad[8 + LEN - 1 : 8 + LEN, :]
    tail = (own == last).astype(F32)
    weight = jnp.exp(total - cum) * tail[:, :HEADS]
    expand = head_expand()
    step_x = mm(step, expand, HIGH)
    weight_x = mm(weight, expand, HIGH)
    taps_b = btaps[...].astype(F32)
    taps_c = ctaps[...].astype(F32)
    taps_m = jnp.concatenate([taps_b, taps_c], axis=1)
    both = conv(mpad, taps_m, masks, 0, 2 * NS)
    bc = both[:, 0:NS]
    bc_out[...] = bc
    cc_out[...] = both[:, NS:]
    bt = jnp.transpose(bc.astype(F32)).astype(BF16)
    taps_v = vtaps[...].astype(F32)
    passing = (last == dpad[7:8, :]).astype(F32)
    factor = mm(jnp.exp(total) * passing[:, :HEADS], expand, HIGH)
    for q in range(4):
        lo = q * 256
        vc = conv(vpad, taps_v, masks, lo, 256)
        vc_out[:, lo : lo + 256] = vc
        xs = (step_x[:, lo : lo + 256] * vc.astype(F32)).astype(BF16)
        xs_out[:, lo : lo + 256] = xs
        ev = (weight_x[:, lo : lo + 256] * xs.astype(F32)).astype(BF16)
        pay[q, 0:NS, :] = mm(bt, ev).astype(BF16)
        hi, low = split2(factor[:, lo : lo + 256])
        rows = iota((8, 256), 0)
        pay[q, NS:PAY, :] = jnp.where(
            rows == 0, hi.astype(F32), jnp.where(rows == 1, low.astype(F32), 0.0)
        ).astype(BF16)


def row_prefix(got):
    states = [got[x, 0:NS, :].astype(F32) for x in range(4)]
    factors = [
        got[x, NS:PAY, :].astype(F32)[0:1] + got[x, NS:PAY, :].astype(F32)[1:2] for x in range(4)
    ]
    before = [None]
    passed = [jnp.ones_like(factors[0])]
    run, gain = states[0], factors[0]
    for x in range(1, 4):
        before.append(run)
        passed.append(gain)
        run = states[x] + factors[x] * run
        gain = factors[x] * gain
    return before, passed, run, gain


def row_total_kernel(got, out):
    _, _, run, gain = row_prefix(got)
    out[0:NS, :] = run.astype(BF16)
    hi, low = split2(gain)
    rows = iota((8, 256), 0)
    out[NS:PAY, :] = jnp.where(
        rows == 0, hi.astype(F32), jnp.where(rows == 1, low.astype(F32), 0.0)
    ).astype(BF16)


def row_carry_kernel(got, one, two, out):
    before, passed, _, _ = row_prefix(got)
    tail = one[NS:PAY, :].astype(F32)
    carry = one[0:NS, :].astype(F32) + (tail[0:1] + tail[1:2]) * two[0:NS, :].astype(F32)
    out[0] = carry.astype(BF16)
    for x in range(1, 4):
        out[x] = (before[x] + passed[x] * carry).astype(BF16)


def inner_kernel(
    xs, vc, bc, cc, docs, docs_row, edges, step_pre, extra, rate, direct, gate,
    p_out, g_out,
    lpad, cum_t,
):
    _, logd = logs(step_pre, extra, rate)
    lpad[...] = jnp.zeros_like(lpad)
    lpad[:, 0:HEADS] = logd
    cum = cumulated(lpad[...])
    cum_t[...] = jnp.transpose(cum)
    expand = head_expand()
    own = docs[...]
    prev = edges[:, CH + 2 * NS :].astype(F32)[7:8, :]
    enter = jnp.exp(cum[:, :HEADS]) * (own == prev).astype(F32)[:, :HEADS]
    enter_x = mm(enter, expand, HIGH)
    mid = cum[BLK - 1 : BLK, :HEADS]
    mid_doc = own[BLK - 1 : BLK, :]
    w0 = jnp.exp(mid - cum[0:BLK, :HEADS]) * (own[0:BLK, :HEADS] == mid_doc[:, :HEADS]).astype(F32)
    w0_x = mm(w0, expand, HIGH)
    r1 = jnp.exp(cum[BLK:, :HEADS] - mid) * (own[BLK:, :HEADS] == mid_doc[:, :HEADS]).astype(F32)
    r1_x = mm(r1, expand, HIGH)
    ev0 = (w0_x * xs[0:BLK, :].astype(F32)).astype(BF16)
    bt0 = jnp.transpose(bc[0:BLK, :].astype(F32)).astype(BF16)
    state0 = mm(bt0, ev0).astype(BF16)
    direct_x = mm(direct[...], expand, HIGH)
    lane = iota((BLK, 2 * HD), 1)
    for b in range(2):
        rows = slice(b * BLK, (b + 1) * BLK)
        cb = cc[rows, :]
        scores = lax.dot_general(
            cb, bc[rows, :], (((1,), (1,)), ((), ())), preferred_element_type=F32
        )
        allowed = (iota((BLK, BLK), 0) >= iota((BLK, BLK), 1)) & (
            own[rows, :] == docs_row[b : b + 1, :]
        )
        bias = jnp.where(allowed, 0.0, NEG)
        for j in range(CH // (2 * HD)):
            cols = slice(j * 128, (j + 1) * 128)
            chunk = xs[rows, cols]
            parts = []
            for h in (2 * j, 2 * j + 1):
                spread = cum[rows, h : h + 1] - cum_t[h : h + 1, rows]
                weighted = (scores * jnp.exp(spread + bias)).astype(BF16)
                parts.append(mm(weighted, chunk))
            y = jnp.where(lane < HD, parts[0], parts[1])
            if b == 1:
                y = y + mm(cb, state0[:, cols]) * r1_x[:, cols]
            y = y + vc[rows, cols].astype(F32) * direct_x[:, cols]
            act = silu(gate[rows, cols].astype(F32))
            p_out[rows, cols] = y * act
            g_out[rows, cols] = act * enter_x[rows, cols]


def outer_kernel(cc, state, p, g, keep, send):
    core = lax.axis_index("tp")

    def half(b, out):
        rows = slice(b * BLK, (b + 1) * BLK)
        for q in range(4):
            cols = slice(q * 256, (q + 1) * 256)
            read = mm(cc[rows, :], state[q])
            out[:, cols] = (p[rows, cols] + g[rows, cols] * read).astype(BF16)

    @pl.when(core == 0)
    def _():
        half(0, keep)
        half(1, send)

    @pl.when(core == 1)
    def _():
        half(1, keep)
        half(0, send)


def route_kernel(chosen, chosen_w, group_w, col_out, row_out):
    lanes = iota((128, EXPERTS), 1)
    hot = [(chosen[:, k : k + 1] == lanes).astype(F32) for k in range(2)]
    below = (iota((128, 128), 0) > iota((128, 128), 1)).astype(BF16)
    rank = mm(below, (hot[0] + hot[1]).astype(BF16))
    out = jnp.zeros((128, 128), F32)
    for k in range(2):
        index = chosen[:, k : k + 1]
        slot = index.astype(F32) * CAP + jnp.sum(rank * hot[k], axis=1, keepdims=True)
        weight = jnp.zeros((128, 1), F32)
        for g in range(4):
            weight = weight + jnp.where((index >> 5) == g, group_w[:, g : g + 1], 0.0)
        weight = weight * chosen_w[:, k : k + 1]
        out = jnp.where(lanes == k, slot, out)
        out = jnp.where(lanes == 2 + k, weight, out)
    col_out[...] = out
    row_out[...] = jnp.transpose(out)[0:8, :]


def unpack_matrix():
    out = iota((256, 256), 0)
    r = iota((256, 256), 1)
    return (out == ((r >> 2) & 3) * 64 + (r >> 4) * 4 + (r & 3)).astype(BF16)


def pack_matrix():
    r = iota((256, 256), 0)
    src = iota((256, 256), 1)
    return (src == ((r >> 2) & 3) * 64 + (r >> 4) * 4 + (r & 3)).astype(BF16)


def proj_kernel(
    keep, got, w_hbm, gain, residual, gain2, route,
    mixed_out, out,
    w, ybuf, sem,
):
    core = lax.axis_index("tp")
    order = [core, 1 - core]
    copies = []
    for i in range(4):
        start = pl.multiple_of(order[i // 2] * CH + (i % 2) * 512, 512)
        copy = pltpu.make_async_copy(
            w_hbm.at[pl.ds(start, 512), :], w.at[pl.ds(i * 512, 512), :], sem.at[i]
        )
        copy.start()
        copies.append(copy)
    a = keep[...].astype(F32)
    b = got[...].astype(F32)
    squares = jnp.sum(a * a, axis=1, keepdims=True) + jnp.sum(b * b, axis=1, keepdims=True)
    factor = lax.rsqrt(squares * (1.0 / D) + EPS)
    ga = gain[pl.ds(core, 1), :]
    gb = gain[pl.ds(1 - core, 1), :]
    na = (a * factor * ga).astype(BF16)
    nb = (b * factor * gb).astype(BF16)
    total = residual[...].astype(F32)
    for i in range(4):
        part = (na, nb)[i // 2][:, (i % 2) * 512 : (i % 2 + 1) * 512]
        copies[i].wait()
        total = total + mm(part, w[i * 512 : (i + 1) * 512, :])
    mixed = total.astype(BF16)
    mixed_out[...] = mixed
    wide = mixed.astype(F32)
    mean = jnp.sum(wide * wide, axis=1, keepdims=True) * (1.0 / D)
    rows_in = (wide * lax.rsqrt(mean + EPS) * gain2[...]).astype(BF16)
    slots = iota((SLOTS, 128), 0).astype(F32)
    hot = (slots == route[0:1, :]) | (slots == route[1:2, :])
    ybuf[...] = mm(hot.astype(BF16), rows_in).astype(BF16)
    pack = pack_matrix()
    for blk in range(8):
        rows = slice(blk * 64, (blk + 1) * 64)
        stacked = jnp.concatenate(
            [ybuf[rows, q * QW : (q + 1) * QW] for q in range(4)], axis=0
        )
        out[blk * 256 : (blk + 1) * 256, :] = mm(pack, stacked).astype(BF16)


def expert_kernel(
    arrived, gate_hbm, up_hbm, down_hbm,
    out,
    wg, wu, wd, x, sem,
):
    copies = [
        pltpu.make_async_copy(src.at[0], dst, sem.at[i])
        for i, (src, dst) in enumerate(((gate_hbm, wg), (up_hbm, wu), (down_hbm, wd)))
    ]
    for copy in copies:
        copy.start()
    unpack = unpack_matrix()
    for blk in range(8):
        flat = mm(unpack, arrived[blk * 256 : (blk + 1) * 256, :]).astype(BF16)
        for q in range(4):
            x[blk * 64 : (blk + 1) * 64, q * QW : (q + 1) * QW] = flat[q * 64 : (q + 1) * 64, :]
    for copy in copies:
        copy.wait()
    pack = pack_matrix()
    for half in range(2):
        rows = slice(half * 256, (half + 1) * 256)
        g = mm(x[rows, :], wg[...])
        u = mm(x[rows, :], wu[...])
        hidden = (silu(g) * u).astype(BF16)
        y = mm(hidden, wd[...]).astype(BF16)
        for i in range(4):
            stacked = jnp.concatenate(
                [y[i * 64 : (i + 1) * 64, q * QW : (q + 1) * QW] for q in range(4)], axis=0
            )
            blk = half * 4 + i
            out[blk * 256 : (blk + 1) * 256, :] = mm(pack, stacked).astype(BF16)


def combine_kernel(back, mixed, route, out, r):
    unpack = unpack_matrix()
    for blk in range(8):
        flat = mm(unpack, back[blk * 256 : (blk + 1) * 256, :]).astype(BF16)
        for q in range(4):
            r[blk * 64 : (blk + 1) * 64, q * QW : (q + 1) * QW] = flat[q * 64 : (q + 1) * 64, :]
    slots = iota((128, SLOTS), 1).astype(F32)
    info = route[...]
    q_mat = jnp.where(slots == info[:, 0:1], info[:, 2:3], 0.0) + jnp.where(
        slots == info[:, 1:2], info[:, 3:4], 0.0
    )
    hi, low = split2(q_mat)
    for q in range(4):
        cols = slice(q * QW, (q + 1) * QW)
        acc = mm(hi, r[:, cols]) + mm(low, r[:, cols])
        out[:, cols] = (mixed[:, cols].astype(F32) + acc).astype(BF16)


def shifted(block, distance):
    count = 1
    for axis in SP:
        count *= lax.axis_size(axis)
    return lax.ppermute(block, SP, [(i, i + distance) for i in range(count - distance)])


def local(
    mixer_value_rows,
    input_map_rows,
    output_map_rows,
    gate_preactivation,
    step_preactivation,
    position_extra_decay,
    head_decay_rate,
    head_direct_term,
    value_taps,
    input_map_taps,
    output_map_taps,
    document_index,
    gated_norm_gain,
    residual,
    mixer_output_weight,
    expert_norm_gain,
    expert_group_weight,
    chosen_expert_weight,
    chosen_expert_index,
    expert_gate_weight,
    expert_up_weight,
    expert_down_weight,
):
    marks = (document_index + 1).astype(F32)
    docs = jnp.broadcast_to(marks[:, None], (LEN, 128))
    docs_row = marks.reshape(2, 128)
    edge = jnp.concatenate(
        [
            mixer_value_rows[-8:],
            input_map_rows[-8:],
            output_map_rows[-8:],
            docs[-8:].astype(BF16),
        ],
        axis=1,
    )
    edges = shifted(edge, 1)
    rate = head_decay_rate.reshape(1, HEADS)
    direct = head_direct_term.reshape(1, HEADS)
    route_col, route_row = call(
        route_kernel, (sds((128, 128), F32), sds((8, 128), F32)), 3, name="route"
    )(chosen_expert_index, chosen_expert_weight, expert_group_weight)
    pay, xs, vc, bc, cc = call(
        conv_kernel,
        (
            sds((4, PAY, 256), BF16),
            sds((LEN, CH), BF16),
            sds((LEN, CH), BF16),
            sds((LEN, NS), BF16),
            sds((LEN, NS), BF16),
        ),
        11,
        scratch=(
            pltpu.VMEM((LEN + 8, CH), F32),
            pltpu.VMEM((LEN + 8, 2 * NS), F32),
            pltpu.VMEM((LEN + 8, 128), F32),
        ),
        name="conv",
    )(
        mixer_value_rows, input_map_rows, output_map_rows, edges, docs,
        step_preactivation, position_extra_decay, rate,
        value_taps, input_map_taps, output_map_taps,
    )
    got = lax.all_to_all(pay, ROW, 0, 0, tiled=True)
    total = call(row_total_kernel, sds((PAY, 256), BF16), 1, name="row_total")(got)
    one, two = shifted(total, 4), shifted(total, 8)
    p, g = call(
        inner_kernel,
        (sds((LEN, CH), F32), sds((LEN, CH), F32)),
        12,
        scratch=(pltpu.VMEM((LEN, 128), F32), pltpu.VMEM((128, LEN), F32)),
        cost=pl.CostEstimate(flops=4_000_000_000, bytes_accessed=4_000_000, transcendentals=0),
        name="inner",
    )(
        xs, vc, bc, cc, docs, docs_row, edges, step_preactivation, position_extra_decay,
        rate, direct, gate_preactivation,
    )
    carried = call(row_carry_kernel, sds((4, NS, 256), BF16), 3, name="row_carry")(got, one, two)
    state = lax.all_to_all(carried, ROW, 0, 0, tiled=True)
    keep, send = call(
        outer_kernel, (sds((BLK, CH), BF16), sds((BLK, CH), BF16)), 4, name="outer"
    )(cc, state, p, g)
    other = lax.ppermute(send, "tp", [(0, 1), (1, 0)])
    mixed, outgoing = call(
        proj_kernel,
        (sds((128, D), BF16), sds((EXPERTS * 16, QW), BF16)),
        7,
        scratch=(
            pltpu.VMEM((D, D), BF16),
            pltpu.VMEM((SLOTS, D), BF16),
            pltpu.SemaphoreType.DMA((4,)),
        ),
        in_specs=vmem(2) + [pl.BlockSpec(memory_space=pl.ANY)] + vmem(4),
        name="proj",
    )(
        keep, other, mixer_output_weight, gated_norm_gain.reshape(2, CH), residual,
        expert_norm_gain.reshape(1, D), route_row,
    )
    arrived = lax.all_to_all(outgoing.reshape(EXPERTS, 16, QW), SP_TP, 0, 0, tiled=True)
    finished = call(
        expert_kernel,
        sds((EXPERTS * 16, QW), BF16),
        4,
        scratch=(
            pltpu.VMEM((D, HID), BF16),
            pltpu.VMEM((D, HID), BF16),
            pltpu.VMEM((HID, D), BF16),
            pltpu.VMEM((SLOTS, D), BF16),
            pltpu.SemaphoreType.DMA((3,)),
        ),
        in_specs=vmem(1) + [pl.BlockSpec(memory_space=pl.ANY)] * 3,
        name="expert",
    )(arrived.reshape(EXPERTS * 16, QW), expert_gate_weight, expert_up_weight, expert_down_weight)
    returned = lax.all_to_all(finished.reshape(EXPERTS, 16, QW), SP_TP, 0, 0, tiled=True)
    return call(
        combine_kernel,
        sds((128, D), BF16),
        3,
        scratch=(pltpu.VMEM((SLOTS, D), BF16),),
        name="combine",
    )(returned.reshape(EXPERTS * 16, QW), mixed, route_col)


def solution(mesh):
    torus = Mesh(mesh.devices.reshape(4, 4, 4, mesh.shape["tp"]), ("sp_0", "sp_1", "sp_2", "tp"))
    in_specs = (
        P(SP, "tp"),
        P(SP, "tp"),
        P(SP, "tp"),
        P(SP, "tp"),
        P(SP, "tp"),
        P(SP, "tp"),
        P("tp"),
        P("tp"),
        P(None, "tp"),
        P(None, "tp"),
        P(None, "tp"),
        P(SP),
        P(),
        P(SP_TP, None),
        P(),
        P(),
        P(SP_TP, None),
        P(SP_TP, None),
        P(SP_TP, None),
        P(SP_TP, None, None),
        P(SP_TP, None, None),
        P(SP_TP, None, None),
    )
    out_specs = P(SP_TP, None)
    return jax.shard_map(local, mesh=torus, in_specs=in_specs, out_specs=out_specs, check_vma=False)
```
